32 devices in a mesh: grp: 2 (over y), sp: 8 (over z, core), tp: 2 (over x).
Axes of the slice: x: 2, y: 2, z: 4, core: 2. Of those that a mesh axis runs over, the one named last changes fastest.
Arguments:
- query_plain: bfloat16 [2560, 1024], P(('grp', 'sp'), 'tp'), parts along dimension 0, may hold values from -6 to 6
- query_turn: bfloat16 [2560, 512], P(('grp', 'sp'), 'tp'), parts along dimension 0, may hold values from -40 to 40, as said below
- latent: bfloat16 [2560, 512], P(('grp', 'sp')), parts along dimension 0, may hold values from -6 to 6
- key_turn: bfloat16 [2560, 64], P(('grp', 'sp')), parts along dimension 0, may hold values from -40 to 40, as said below
- latent_norm_scale: bfloat16 [512], replicated, may hold values from 0.099609375 to 1.8984375
- plain_key_matrix: bfloat16 [512, 1024], P(None, 'tp'), may hold values from -0.25 to 0.25
- value_matrix: bfloat16 [512, 1024], P(None, 'tp'), may hold values from -0.25 to 0.25
- residual: bfloat16 [2560, 2048], P(('grp', 'sp', 'tp')), parts along dimension 0, may hold values from -6 to 6
- out_weight: bfloat16 [1024, 2048], replicated, may hold values from -6 to 6
- ffn_gain: bfloat16 [2048], replicated, may hold values from 0.099609375 to 1.8984375
- gate_weight: bfloat16 [8, 2048, 1024], P('sp', None, 'tp'), may hold values from -1 to 1
- up_weight: bfloat16 [8, 2048, 1024], P('sp', None, 'tp'), may hold values from -1 to 1
- down_weight: bfloat16 [8, 1024, 2048], P('sp', 'tp'), may hold values from -0.0625 to 0.0625
- routes: int32 [2560, 4], P(('grp', 'sp', 'tp')), parts along dimension 0, may hold values from 0 to 7, all different within a row; in each aligned block of 80 rows (0 to 79, 80 to 159, ...) at most 60 rows name the same one
- route_weights: float32 [2560, 4], P(('grp', 'sp', 'tp')), parts along dimension 0, may hold values from 0.1 to 0.6
Outputs:
- mixed: bfloat16 [2560, 2048], P(('grp', 'sp', 'tp')), parts along dimension 0
The draws below stay inside these ranges and needn't reach their ends.
There are 2 independent parts, one for each index of `grp`. The reference program is written for one: setup_inputs(seed, part) draws one part's arguments, and reference() takes and returns one part's arrays. A program takes and returns all parts, laid end to end along the dimension named above; an argument that names none is the same for every part. Nothing has to cross between parts.
Inputs may be any that keep to these rules, and one draw needn't show every extreme that they name: `query_turn`: in the hidden draw some rows are large. `key_turn`: in the hidden draw some rows are large. `routes`: each row names 4 different experts. In each aligned block of 80 rows (the rows of one device) no expert is named more than 60 times, a bound that some block reaches.
All inputs are finite; a program needn't handle non-finite values.
Results may differ from the reference program's by a relative error of at most 0.015.
Values may be sent and summed in bfloat16 or wider, within the bound.
No kernel may reach another device: no remote copies, remote signals or barrier semaphores. Data moves between devices by JAX's collectives and lax.ppermute only.
A program may use at most 128 MiB of HBM per device.

```python
import math
import jax
import jax.numpy as jnp
import numpy as np
from jax import lax

D = 2048
ATTENTION_HEADS = 8
PLAIN_HEAD_WIDTH = 128
QK_ROPE = 64
VALUE_WIDTH = 128
LATENT_WIDTH = 512
D_EXPERT = 1024
TOP = 4
GRID_W = 64
ROWS_DEV = 80
SEQUENCE_TOKENS = 1280
EXPERTS = 8
CAP = 60
N_SP = 8
N_TP = 2


def draw_query_turn(key, part):
    base = jnp.clip(jax.random.normal(jax.random.fold_in(key, 1), (SEQUENCE_TOKENS, ATTENTION_HEADS * QK_ROPE), jnp.float32), -6.0, 6.0)
    return base.astype(jnp.bfloat16)


def draw_key_turn(key, part):
    base = jnp.clip(jax.random.normal(jax.random.fold_in(key, 2), (SEQUENCE_TOKENS, QK_ROPE), jnp.float32), -6.0, 6.0)
    return base.astype(jnp.bfloat16)


def block_scale(own_key, extent, cuts, least, high):
    loudness, own = 1.0, jax.random.fold_in(own_key, 6)
    for dim, shards_of in cuts:
        steps = jnp.exp(jax.random.uniform(jax.random.fold_in(own, dim), (shards_of,), jnp.float32, least / len(cuts), high / len(cuts)))
        loudness = loudness * jnp.repeat(steps, extent[dim] // shards_of).reshape([-1 if axis == dim else 1 for axis in range(len(extent))])
    return loudness


def shared_out(stream_key, own, number, rows, count, top, reach, skew):
    ranking = jax.random.permutation(stream_key, count)
    crowded, common = shares(count, rows * top, reach, skew, True), shares(count, rows * top, reach, skew, False)
    places = jnp.arange(count)

    def named(sizes, offset_by):
        used = int((sizes > 0).sum())
        fixed = max(1, used // 4)
        passed = fixed + (places - fixed + offset_by * (used - fixed)) % max(1, count - fixed)
        return jnp.zeros((count,), jnp.int32).at[ranking[jnp.where(places < fixed, places, passed)]].set(jnp.asarray(sizes, jnp.int32))

    sizes = jnp.where(number % 4 == 0, named(crowded, number // 4), named(common, number - number // 4 - 1))
    mixed = jax.random.permutation(jax.random.fold_in(own, 3), count)
    source_of, sink = mixed[0:count // 2 * 2:2], mixed[1:count // 2 * 2:2]
    slack = jnp.minimum(sizes[source_of] - 1, reach - sizes[sink]) // 2
    slack = jnp.where((source_of == ranking[0]) | (sink == ranking[0]) | (sizes[sink] == 0), 0, jnp.maximum(slack, 0))
    passed = jax.random.randint(jax.random.fold_in(own, 4), (count // 2,), 0, 1 << 20) % (slack + 1)
    sizes = sizes.at[source_of].add(-passed).at[sink].add(passed)
    members = jnp.searchsorted(jnp.cumsum(sizes), jnp.arange(rows * top), side="right").astype(jnp.int32)
    grid = members.reshape(top, rows).T
    grid = grid[jax.random.permutation(jax.random.fold_in(own, 1), rows)]
    offset_by = jax.random.randint(jax.random.fold_in(own, 2), (rows, 1), 0, top)
    return jnp.take_along_axis(grid, (jnp.arange(top)[None, :] + offset_by) % top, axis=1)


def shares(count, total, most, lean, full):
    loads = [(1 << 20) // math.isqrt(standing ** lean) + 1 for standing in range(1, count + 1)]
    largest = most if full else min(most, max(-(-total // count), total * loads[0] // sum(loads)))
    least = 1 if total - largest >= count - 1 else 0
    given, surplus = [largest] + [least] * (count - 1), total - largest - least * (count - 1)
    while surplus > 0:
        candidates = [i for i in range(1, count) if given[i] < largest] or [i for i in range(1, count) if given[i] < most]
        whole, budget = sum([loads[i] for i in candidates]), surplus
        for i in candidates:
            more = min(most - given[i], max(1, budget * loads[i] // whole), surplus)
            given[i] = given[i] + more
            surplus = surplus - more
    return np.array(given)


def scatter_about(own_key, dims, scale, bound, shards=(), kind=jnp.bfloat16):
    drawn = jax.random.normal(own_key, dims, jnp.float32) * scale
    if len(shards) > 0:
        drawn = block_scale(own_key, dims, shards, -0.22, 0.18) * drawn
    return jnp.clip(drawn, min=-bound, max=bound).astype(kind)


def setup_inputs(seed: int = 0, part: int = 0) -> dict:
    arg_keys = jax.random.split(jax.random.key(seed), 16)
    part_keys = jax.random.split(jax.random.fold_in(arg_keys[15], part), 16)
    query_plain = scatter_about(part_keys[0], (SEQUENCE_TOKENS, ATTENTION_HEADS * PLAIN_HEAD_WIDTH), 1.0, 6.0, ((0, 8), (1, 2)))
    query_turn = draw_query_turn(jax.random.fold_in(jax.random.fold_in(arg_keys[15], part), 71), part)
    latent = scatter_about(part_keys[2], (SEQUENCE_TOKENS, LATENT_WIDTH), 1.0, 6.0, ((0, 8),))
    key_turn = draw_key_turn(jax.random.fold_in(jax.random.fold_in(arg_keys[15], part), 71), part)
    latent_norm_scale = jnp.clip(1.0 + 0.18 * jax.random.normal(arg_keys[4], (LATENT_WIDTH,), jnp.float32), 0.099609375, 1.8984375).astype(jnp.bfloat16)
    plain_key_matrix = scatter_about(arg_keys[5], (LATENT_WIDTH, ATTENTION_HEADS * PLAIN_HEAD_WIDTH), LATENT_WIDTH ** -0.5, 0.25, ((1, 2),))
    value_matrix = scatter_about(arg_keys[6], (LATENT_WIDTH, ATTENTION_HEADS * VALUE_WIDTH), LATENT_WIDTH ** -0.5, 0.25, ((1, 2),))
    residual = scatter_about(part_keys[7], (SEQUENCE_TOKENS, D), 1.0, 6.0, ((0, 16),))
    out_weight = scatter_about(arg_keys[8], (ATTENTION_HEADS * VALUE_WIDTH, D), (16 * (ATTENTION_HEADS * VALUE_WIDTH) ** -0.5), 6.0)
    ffn_gain = jnp.clip(1.0 + 0.18 * jax.random.normal(arg_keys[9], (D,), jnp.float32), 0.099609375, 1.8984375).astype(jnp.bfloat16)
    gate_weight = scatter_about(arg_keys[10], (EXPERTS, D, D_EXPERT), (3 * D ** -0.5), 1.0, ((0, 8), (2, 2)))
    up_weight = scatter_about(arg_keys[11], (EXPERTS, D, D_EXPERT), (3 * D ** -0.5), 1.0, ((0, 8), (2, 2)))
    down_weight = scatter_about(arg_keys[12], (EXPERTS, D_EXPERT, D), (0.15 * D_EXPERT ** -0.5), 0.0625, ((0, 8), (1, 2)))
    routes_keys = jax.random.split(jax.random.fold_in(part_keys[13], 1), SEQUENCE_TOKENS // ROWS_DEV)
    routes_turns = jax.random.permutation(jax.random.fold_in(part_keys[13], 3), SEQUENCE_TOKENS // ROWS_DEV)
    routes = jax.vmap(lambda own, number: shared_out(jax.random.fold_in(part_keys[13], 2), own, number, ROWS_DEV, EXPERTS, TOP, CAP, 1))(routes_keys, routes_turns).reshape((SEQUENCE_TOKENS, TOP))
    route_weights = jnp.clip(0.1 + 0.5 * jax.random.uniform(part_keys[14], (SEQUENCE_TOKENS, TOP), jnp.float32) ** block_scale(part_keys[14], (SEQUENCE_TOKENS, TOP), ((0, 16),), -0.2, 0.2), 0.1, 0.6)
    return dict(query_plain=query_plain, query_turn=query_turn, latent=latent, key_turn=key_turn, latent_norm_scale=latent_norm_scale, plain_key_matrix=plain_key_matrix, value_matrix=value_matrix, residual=residual, out_weight=out_weight, ffn_gain=ffn_gain, gate_weight=gate_weight, up_weight=up_weight, down_weight=down_weight, routes=routes, route_weights=route_weights)


theta = 10000.0
eps = 1e-06
limit = 7.0
slope = 1.702

def turn(vector, row_shift, col_shift):
    width = vector.shape[-1]
    count = width // 4
    half = width // 2
    freqs = theta ** (-jnp.arange(count, dtype=jnp.float32) / count)
    extra = (1,) * (vector.ndim - 2)
    pieces = []
    for portion, shift in ((vector[..., :half], row_shift), (vector[..., half:], col_shift)):
        angle = (shift.astype(jnp.float32)[:, None] * freqs[None, :]).reshape((shift.shape[0],) + extra + (count,))
        lower = portion[..., :count]
        upper = portion[..., count:]
        pieces.append(jnp.concatenate([lower * jnp.cos(angle) - upper * jnp.sin(angle), lower * jnp.sin(angle) + upper * jnp.cos(angle)], axis=-1))
    return jnp.concatenate(pieces, axis=-1)

def norm_scale(values, gain):
    wide = values.astype(jnp.float32)
    return wide * lax.rsqrt(lax.optimization_barrier(jnp.mean(wide * wide, axis=-1, keepdims=True)) + eps) * gain.astype(jnp.float32)

def expert_apply(operands):
    rows, gate_w, up_w, down_w = operands
    gate_pre = jnp.minimum(jnp.dot(rows, gate_w, preferred_element_type=jnp.float32), limit)
    up_pre = jnp.clip(jnp.dot(rows, up_w, preferred_element_type=jnp.float32), -limit, limit)
    active = ((up_pre + 1.0) * gate_pre * jax.nn.sigmoid(slope * gate_pre)).astype(jnp.bfloat16)
    piece = down_w.shape[0] // N_TP
    groups = jnp.einsum('rnp,npd->nrd', active.reshape(rows.shape[0], N_TP, piece).astype(jnp.float32), down_w.reshape(N_TP, piece, down_w.shape[1]).astype(jnp.float32))
    rounded = lax.optimization_barrier(groups.astype(jnp.bfloat16))
    return lax.optimization_barrier(jnp.sum(rounded.astype(jnp.float32), axis=0)).astype(jnp.bfloat16)

def reference(query_plain, query_turn, latent, key_turn, latent_norm_scale, plain_key_matrix, value_matrix, residual, out_weight, ffn_gain, gate_weight, up_weight, down_weight, routes, route_weights):
    place = jnp.arange(SEQUENCE_TOKENS, dtype=jnp.int32)
    grid_row = place // GRID_W
    grid_col = place % GRID_W
    normed_latent = norm_scale(latent, latent_norm_scale).astype(jnp.bfloat16)
    key_plain = jnp.dot(normed_latent, plain_key_matrix, preferred_element_type=jnp.float32).astype(jnp.bfloat16)
    values = jnp.dot(normed_latent, value_matrix, preferred_element_type=jnp.float32).astype(jnp.bfloat16)
    key_rot = turn(key_turn.astype(jnp.float32), grid_row, grid_col).astype(jnp.bfloat16)
    query_rot = turn(query_turn.astype(jnp.float32).reshape(SEQUENCE_TOKENS, ATTENTION_HEADS, QK_ROPE), grid_row, grid_col).astype(jnp.bfloat16)
    plain_heads = jnp.moveaxis(query_plain.reshape(SEQUENCE_TOKENS, ATTENTION_HEADS, PLAIN_HEAD_WIDTH), 1, 0)
    rot_heads = jnp.moveaxis(query_rot, 1, 0)
    key_heads = jnp.moveaxis(key_plain.reshape(SEQUENCE_TOKENS, ATTENTION_HEADS, PLAIN_HEAD_WIDTH), 1, 0)
    value_heads = jnp.moveaxis(values.reshape(SEQUENCE_TOKENS, ATTENTION_HEADS, VALUE_WIDTH), 1, 0)
    scale = (PLAIN_HEAD_WIDTH + QK_ROPE) ** (-0.5)
    block = math.gcd(SEQUENCE_TOKENS, 512)

    def one_head(operands):
        head_plain, head_rot, head_keys, head_values = operands

        def one_block(start):
            block_plain = lax.dynamic_slice_in_dim(head_plain, start, block, 0)
            block_rot = lax.dynamic_slice_in_dim(head_rot, start, block, 0)
            scores = (jnp.einsum('qd,kd->qk', block_plain, head_keys, preferred_element_type=jnp.float32) + jnp.einsum('qd,kd->qk', block_rot, key_rot, preferred_element_type=jnp.float32)) * scale
            peak = lax.optimization_barrier(jnp.max(scores, axis=1, keepdims=True))
            weights = jnp.exp(scores - peak)
            summed = jnp.dot(weights.astype(jnp.bfloat16), head_values, preferred_element_type=jnp.float32)
            return (summed / lax.optimization_barrier(jnp.sum(weights, axis=1, keepdims=True))).astype(jnp.bfloat16)
        starts = jnp.arange(SEQUENCE_TOKENS // block, dtype=jnp.int32) * block
        return lax.map(one_block, starts).reshape(SEQUENCE_TOKENS, VALUE_WIDTH)
    attended = lax.map(one_head, (plain_heads, rot_heads, key_heads, value_heads))
    attended = jnp.moveaxis(attended, 0, 1).reshape(SEQUENCE_TOKENS, ATTENTION_HEADS * VALUE_WIDTH)
    hidden = (residual.astype(jnp.float32) + jnp.dot(attended, out_weight, preferred_element_type=jnp.float32)).astype(jnp.bfloat16)
    normed = norm_scale(hidden, ffn_gain).astype(jnp.bfloat16)
    blocks = N_SP * N_TP
    per_block = routes.reshape(blocks, ROWS_DEV * TOP)
    marks = (per_block[..., None] == jnp.arange(EXPERTS, dtype=jnp.int32)).astype(jnp.int32)
    earlier = jnp.cumsum(marks, axis=1, dtype=jnp.int32) - marks
    slots = lax.optimization_barrier(jnp.sum(earlier * marks, axis=2, dtype=jnp.int32))
    target = ((per_block * blocks + jnp.arange(blocks, dtype=jnp.int32)[:, None]) * CAP + slots).reshape(SEQUENCE_TOKENS * TOP)
    copies = jnp.repeat(normed, TOP, axis=0)
    buffer = jnp.zeros((EXPERTS * blocks * CAP, D), jnp.bfloat16).at[target].set(copies)
    results = lax.map(expert_apply, (buffer.reshape(EXPERTS, blocks * CAP, D), gate_weight, up_weight, down_weight))
    results = results.reshape(EXPERTS * blocks * CAP, D)
    picked = results[target].reshape(SEQUENCE_TOKENS, TOP, D).astype(jnp.float32)
    return (hidden.astype(jnp.float32) + lax.optimization_barrier(jnp.sum(route_weights[..., None] * picked, axis=1))).astype(jnp.bfloat16)
```

```python
import functools

import jax
import jax.numpy as jnp
from jax import lax
from jax.experimental import pallas as pl
from jax.experimental.pallas import tpu as pltpu
from jax.sharding import PartitionSpec as P

PLAIN_HEAD_WIDTH = 128
QK_ROPE = 64
VALUE_WIDTH = 128
GRID_W = 64


theta = 10000.0
eps = 1e-06
limit = 7.0
slope = 1.702


def turn(vector, row_shift, col_shift):
    width = vector.shape[-1]
    count = width // 4
    half = width // 2
    freqs = theta ** (-jnp.arange(count, dtype=jnp.float32) / count)
    extra = (1,) * (vector.ndim - 2)
    pieces = []
    for portion, shift in ((vector[..., :half], row_shift), (vector[..., half:], col_shift)):
        angle = (shift.astype(jnp.float32)[:, None] * freqs[None, :]).reshape(
            (shift.shape[0],) + extra + (count,)
        )
        lower = portion[..., :count]
        upper = portion[..., count:]
        pieces.append(
            jnp.concatenate(
                [
                    lower * jnp.cos(angle) - upper * jnp.sin(angle),
                    lower * jnp.sin(angle) + upper * jnp.cos(angle),
                ],
                axis=-1,
            )
        )
    return jnp.concatenate(pieces, axis=-1)


def norm_scale(values, gain):
    wide = values.astype(jnp.float32)
    return (
        wide
        * lax.rsqrt(jnp.mean(wide * wide, axis=-1, keepdims=True) + eps)
        * gain.astype(jnp.float32)
    )


def expert_active(rows, gate_w, up_w):
    gate_pre = jnp.minimum(jnp.dot(rows, gate_w, preferred_element_type=jnp.float32), limit)
    up_pre = jnp.clip(jnp.dot(rows, up_w, preferred_element_type=jnp.float32), -limit, limit)
    return ((up_pre + 1.0) * gate_pre * jax.nn.sigmoid(slope * gate_pre)).astype(jnp.bfloat16)


def expert_whole(rows, gate_w, up_w, down_w, groups):
    active = expert_active(rows, gate_w, up_w)
    piece = down_w.shape[0] // groups
    total = jnp.zeros((rows.shape[0], down_w.shape[1]), jnp.float32)
    for index in range(groups):
        product = jnp.dot(
            active[:, index * piece : (index + 1) * piece],
            down_w[index * piece : (index + 1) * piece],
            preferred_element_type=jnp.float32,
        )
        total = total + product.astype(jnp.bfloat16).astype(jnp.float32)
    return total.astype(jnp.bfloat16)


def routed_on_device(
    query_plain,
    query_turn,
    latent,
    key_turn,
    latent_norm_scale,
    plain_key_matrix,
    value_matrix,
    residual,
    out_weight,
    ffn_gain,
    gate_weight,
    up_weight,
    down_weight,
    routes,
    route_weights,
):
    tok_dev = latent.shape[0]
    heads_dev = query_plain.shape[1] // PLAIN_HEAD_WIDTH
    model_width = residual.shape[1]
    place = lax.axis_index("sp") * tok_dev + jnp.arange(tok_dev, dtype=jnp.int32)
    grid_row = place // GRID_W
    grid_col = place % GRID_W
    normed_latent = norm_scale(latent, latent_norm_scale).astype(jnp.bfloat16)
    key_plain = jnp.dot(normed_latent, plain_key_matrix, preferred_element_type=jnp.float32).astype(
        jnp.bfloat16
    )
    values = jnp.dot(normed_latent, value_matrix, preferred_element_type=jnp.float32).astype(
        jnp.bfloat16
    )
    key_rot = turn(key_turn.astype(jnp.float32), grid_row, grid_col).astype(jnp.bfloat16)
    key_pairs = key_rot.reshape(tok_dev // 2, 2 * QK_ROPE)
    query_rot = turn(
        query_turn.astype(jnp.float32).reshape(tok_dev, heads_dev, QK_ROPE), grid_row, grid_col
    ).astype(jnp.bfloat16)
    plain_query = query_plain.reshape(tok_dev, heads_dev, PLAIN_HEAD_WIDTH)
    scale = (PLAIN_HEAD_WIDTH + QK_ROPE) ** (-0.5)
    most = jnp.full((heads_dev, tok_dev), -jnp.inf, jnp.float32)
    total = jnp.zeros((heads_dev, tok_dev), jnp.float32)
    summed = jnp.zeros((heads_dev, tok_dev, VALUE_WIDTH), jnp.float32)
    piece_keys = lax.all_gather(key_plain, "sp", axis=0, tiled=True)
    piece_values = lax.all_gather(values, "sp", axis=0, tiled=True)
    piece_pairs = lax.all_gather(key_pairs, "sp", axis=0, tiled=True)
    count = piece_keys.shape[0]
    piece_rot = piece_pairs.reshape(count, QK_ROPE)
    new_most = []
    new_total = []
    new_summed = []
    for head in range(heads_dev):
        head_keys = piece_keys[:, head * PLAIN_HEAD_WIDTH : (head + 1) * PLAIN_HEAD_WIDTH]
        head_values = piece_values[:, head * VALUE_WIDTH : (head + 1) * VALUE_WIDTH]
        scores = (
            jnp.einsum(
                "qd,kd->qk", plain_query[:, head], head_keys, preferred_element_type=jnp.float32
            )
            + jnp.einsum(
                "qd,kd->qk", query_rot[:, head], piece_rot, preferred_element_type=jnp.float32
            )
        ) * scale
        peak = jnp.max(scores, axis=1)
        factor = jnp.exp(most[head] - peak)
        weights = jnp.exp(scores - peak[:, None])
        new_total.append(total[head] * factor + jnp.sum(weights, axis=1))
        new_summed.append(
            summed[head] * factor[:, None]
            + jnp.dot(weights.astype(jnp.bfloat16), head_values, preferred_element_type=jnp.float32)
        )
        new_most.append(peak)
    total = jnp.stack(new_total)
    summed = jnp.stack(new_summed)
    attended = jnp.transpose((summed / total[..., None]).astype(jnp.bfloat16), (1, 0, 2)).reshape(
        tok_dev, heads_dev * VALUE_WIDTH
    )
    rows_dev = residual.shape[0]
    own_rows = lax.dynamic_slice_in_dim(
        out_weight, lax.axis_index("tp") * heads_dev * VALUE_WIDTH, heads_dev * VALUE_WIDTH, 0
    )
    projected = lax.psum_scatter(
        jnp.dot(attended, own_rows, preferred_element_type=jnp.float32).astype(jnp.bfloat16),
        "tp",
        scatter_dimension=0,
        tiled=True,
    ).astype(jnp.float32)
    hidden = (residual.astype(jnp.float32) + projected).astype(jnp.bfloat16)
    normed = norm_scale(hidden, ffn_gain).astype(jnp.bfloat16)
    top_count = routes.shape[1]
    experts_all = lax.axis_size("sp") * gate_weight.shape[0]
    capacity = min(rows_dev, max(2, rows_dev * top_count * 3 // (2 * experts_all)))
    flat_routes = routes.reshape(rows_dev * top_count)
    marks = (flat_routes[:, None] == jnp.arange(experts_all, dtype=jnp.int32)[None, :]).astype(
        jnp.int32
    )
    earlier = jnp.cumsum(marks, axis=0, dtype=jnp.int32) - marks
    slots = jnp.sum(earlier * marks, axis=1, dtype=jnp.int32)
    target = flat_routes * capacity + slots
    chosen = (
        target.reshape(rows_dev, top_count)[None, :, :]
        == jnp.arange(experts_all * capacity, dtype=jnp.int32)[:, None, None]
    )
    dispatch_table = jnp.sum(chosen.astype(jnp.bfloat16), axis=2)
    outgoing = jnp.dot(dispatch_table, normed, preferred_element_type=jnp.float32).astype(
        jnp.bfloat16
    )
    outgoing = outgoing.reshape(experts_all, capacity, model_width)
    gate_w = gate_weight[0]
    up_w = up_weight[0]
    down_w = down_weight[0]
    group = lax.axis_size("tp")
    gate_full, up_full, down_full = (
        lax.all_gather(gate_w, "tp", axis=1, tiled=True),
        lax.all_gather(up_w, "tp", axis=1, tiled=True),
        lax.all_gather(down_w, "tp", axis=0, tiled=True),
    )
    arrived = lax.all_to_all(outgoing, "sp", split_axis=0, concat_axis=0, tiled=True)
    result_rows = expert_whole(
        arrived.reshape(experts_all * capacity, model_width), gate_full, up_full, down_full, group
    )
    returned = lax.all_to_all(
        result_rows.reshape(experts_all, capacity, model_width),
        "sp",
        split_axis=0,
        concat_axis=0,
        tiled=True,
    )
    picked = returned.reshape(experts_all * capacity, model_width)[target]
    picked = picked.reshape(rows_dev, top_count, model_width).astype(jnp.float32)
    return (hidden.astype(jnp.float32) + jnp.sum(route_weights[..., None] * picked, axis=1)).astype(
        jnp.bfloat16
    )


def zshift(value, hops):
    size = lax.axis_size("sp")
    return lax.ppermute(value, "sp", [(i, (i + 2 * hops) % size) for i in range(size)])


def cswap(value):
    return lax.ppermute(value, "sp", [(i, i ^ 1) for i in range(lax.axis_size("sp"))])


def xswap(value):
    return lax.ppermute(value, "tp", [(0, 1), (1, 0)])


def swap_matrix(width):
    row = lax.broadcasted_iota(jnp.int32, (width, width), 0)
    col = lax.broadcasted_iota(jnp.int32, (width, width), 1)
    return (row == (col ^ (QK_ROPE // 4))).astype(jnp.bfloat16)


def turn_table(place):
    count = QK_ROPE // 4
    freqs = theta ** (-jnp.arange(count, dtype=jnp.float32) / count)
    row = (place // GRID_W).astype(jnp.float32)[:, None] * freqs[None, :]
    col = (place % GRID_W).astype(jnp.float32)[:, None] * freqs[None, :]
    angle = jnp.concatenate([row, col], axis=-1)
    cos, sin = jnp.cos(angle), jnp.sin(angle)
    return jnp.concatenate(
        [cos[:, :count], cos[:, :count], cos[:, count:], cos[:, count:]]
        + [-sin[:, :count], sin[:, :count], -sin[:, count:], sin[:, count:]],
        axis=-1,
    )


def attend_kernel(
    first, last, width, at, qp, qr, la, lb, ta, tb, gain, wk, wv, perm, m_in, o_in, *outs
):
    heads = qp.shape[1] // PLAIN_HEAD_WIDTH
    lat = jnp.concatenate([la[:, :width], lb[:, :width]], axis=0).astype(jnp.float32)
    mean = jnp.mean(lat * lat, axis=-1, keepdims=True)
    normed = (lat * lax.rsqrt(mean + eps) * gain[...].astype(jnp.float32)).astype(jnp.bfloat16)
    keys = jnp.dot(normed, wk[...], preferred_element_type=jnp.float32).astype(jnp.bfloat16)
    vals = jnp.dot(normed, wv[...], preferred_element_type=jnp.float32).astype(jnp.bfloat16)
    raw = jnp.concatenate([la[:, width : width + QK_ROPE], lb[:, width : width + QK_ROPE]], axis=0)
    table = jnp.concatenate([ta[...], tb[...]], axis=0)
    swapped = jnp.dot(raw, perm[...], preferred_element_type=jnp.float32)
    rot = (
        raw.astype(jnp.float32) * table[:, :QK_ROPE] + swapped * table[:, QK_ROPE:]
    ).astype(jnp.bfloat16)
    scale = (PLAIN_HEAD_WIDTH + QK_ROPE) ** (-0.5)
    for head in range(heads):
        cols = slice(head * PLAIN_HEAD_WIDTH, (head + 1) * PLAIN_HEAD_WIDTH)
        query = jnp.concatenate(
            [qp[:, cols], qr[:, head * QK_ROPE : (head + 1) * QK_ROPE]], axis=1
        )
        key = jnp.concatenate([keys[:, cols], rot], axis=1)
        scores = (
            lax.dot_general(
                query, key, (((1,), (1,)), ((), ())), preferred_element_type=jnp.float32
            )
            * scale
        )
        peak = jnp.max(scores, axis=1, keepdims=True)
        if not first:
            old = m_in[:, head : head + 1]
            peak = jnp.maximum(peak, old)
        weights = jnp.exp(scores - peak)
        total = jnp.sum(weights, axis=1, keepdims=True)
        summed = jnp.dot(
            weights.astype(jnp.bfloat16), vals[:, cols], preferred_element_type=jnp.float32
        )
        if not first:
            factor = jnp.exp(old - peak)
            total = total + factor * m_in[:, heads + head : heads + head + 1]
            summed = summed + factor * o_in[:, cols]
        if last:
            mine, other, scratch = outs
            scratch[:, cols] = summed / total
        else:
            m_out, o_out = outs
            m_out[:, head : head + 1] = peak
            m_out[:, heads + head : heads + head + 1] = total
            o_out[:, cols] = summed
    if last:
        rows = mine.shape[0]
        side = at[2]
        mine[...] = scratch[pl.ds(pl.multiple_of(side * rows, rows), rows), :].astype(jnp.bfloat16)
        other[...] = scratch[
            pl.ds(pl.multiple_of((1 - side) * rows, rows), rows), :
        ].astype(jnp.bfloat16)


def attend(first, last, at, qp, qr, la, lb, table, gain, wk, wv, perm, m_in, o_in):
    rows, width = qp.shape
    latent_width = wk.shape[0]
    keys = 2 * la.shape[0]

    def whole(array):
        return pl.BlockSpec(array.shape, lambda i, at: (0,) * array.ndim)

    block = (la.shape[0], table.shape[1])
    operands = [qp, qr, la, lb, table, table, gain, wk, wv, perm, m_in, o_in]
    specs = [whole(a) for a in operands]
    specs[4] = pl.BlockSpec(block, lambda i, at: (at[0], 0))
    specs[5] = pl.BlockSpec(block, lambda i, at: (at[1], 0))
    if last:
        shapes = [jax.ShapeDtypeStruct((rows // 2, width), jnp.bfloat16)] * 2
        scratch = [pltpu.VMEM((rows, width), jnp.float32)]
    else:
        shapes = [
            jax.ShapeDtypeStruct((rows, 128), jnp.float32),
            jax.ShapeDtypeStruct((rows, width), jnp.float32),
        ]
        scratch = []
    flops = 2 * keys * latent_width * 2 * width + 2 * rows * keys * (2 * width + qr.shape[1])
    return pl.pallas_call(
        functools.partial(attend_kernel, first, last, latent_width),
        grid_spec=pltpu.PrefetchScalarGridSpec(
            num_scalar_prefetch=1,
            grid=(1,),
            in_specs=specs,
            out_specs=[pl.BlockSpec(s.shape, lambda i, at: (0, 0)) for s in shapes],
            scratch_shapes=scratch,
        ),
        out_shape=shapes,
        compiler_params=pltpu.CompilerParams(vmem_limit_bytes=24 << 20),
        cost_estimate=pl.CostEstimate(
            flops=flops, bytes_accessed=4 << 20, transcendentals=rows * keys * 4
        ),
        name="attend",
    )(at, *operands)


def hidden_kernel(at, mine, other, own_w, other_w, residual, gain, hidden, normed):
    step = pl.program_id(0)
    wide = own_w.shape[1]
    cols = pl.ds(pl.multiple_of(step * wide, wide), wide)
    product = jnp.dot(mine[...], own_w[...], preferred_element_type=jnp.float32)
    product = product + jnp.dot(other[...], other_w[...], preferred_element_type=jnp.float32)
    hidden[:, cols] = (residual[:, cols].astype(jnp.float32) + product).astype(jnp.bfloat16)

    @pl.when(step == pl.num_programs(0) - 1)
    def _():
        value = hidden[...].astype(jnp.float32)
        mean = jnp.mean(value * value, axis=-1, keepdims=True)
        normed[...] = (value * lax.rsqrt(mean + eps) * gain[...].astype(jnp.float32)).astype(
            jnp.bfloat16
        )


def make_hidden(at, mine, other, out_weight, residual, gain):
    rows, width = residual.shape
    part = mine.shape[1]
    steps = 4
    wide = width // steps

    def whole(array):
        return pl.BlockSpec(array.shape, lambda i, at: (0, 0))

    return pl.pallas_call(
        hidden_kernel,
        grid_spec=pltpu.PrefetchScalarGridSpec(
            num_scalar_prefetch=1,
            grid=(steps,),
            in_specs=[
                whole(mine),
                whole(other),
                pl.BlockSpec((part, wide), lambda i, at: (at[2], i)),
                pl.BlockSpec((part, wide), lambda i, at: (1 - at[2], i)),
                whole(residual),
                whole(gain),
            ],
            out_specs=[pl.BlockSpec((rows, width), lambda i, at: (0, 0))] * 2,
        ),
        out_shape=[jax.ShapeDtypeStruct((rows, width), jnp.bfloat16)] * 2,
        compiler_params=pltpu.CompilerParams(vmem_limit_bytes=24 << 20),
        cost_estimate=pl.CostEstimate(
            flops=4 * rows * part * width, bytes_accessed=6 << 20, transcendentals=0
        ),
        name="hidden",
    )(at, mine, other, out_weight, out_weight, residual, gain)


def experts_kernel(xa, xb, wa, wb, g0, u0, d0, g1, u1, d1, ya, yb, acc):
    step = pl.program_id(0)
    rows = jnp.concatenate([xa[...], xb[...]], axis=0)
    scale = jnp.concatenate([wa[...], wb[...]], axis=0)
    total = None
    for index, (g, u, d) in enumerate(((g0, u0, d0), (g1, u1, d1))):
        gate = jnp.minimum(jnp.dot(rows, g[...], preferred_element_type=jnp.float32), limit)
        up = jnp.clip(jnp.dot(rows, u[...], preferred_element_type=jnp.float32), -limit, limit)
        active = ((up + 1.0) * gate * jax.nn.sigmoid(slope * gate)).astype(jnp.bfloat16)
        product = jnp.dot(active, d[...], preferred_element_type=jnp.float32)
        product = product * scale[:, index : index + 1]
        total = product if total is None else total + product

    @pl.when(step == 0)
    def _():
        acc[...] = total

    @pl.when(step > 0)
    def _():
        acc[...] += total

    @pl.when(step == pl.num_programs(0) - 1)
    def _():
        half = xa.shape[0]
        ya[...] = acc[:half, :].astype(jnp.bfloat16)
        yb[...] = acc[half:, :].astype(jnp.bfloat16)


def experts(xa, xb, wa, wb, weights):
    rows, width = xa.shape
    units = weights[0].shape[1]
    steps = 2
    wide = units // steps

    def whole(array):
        return pl.BlockSpec(array.shape, lambda i: (0, 0))

    into = pl.BlockSpec((width, wide), lambda i: (0, i))
    back = pl.BlockSpec((wide, width), lambda i: (i, 0))
    return pl.pallas_call(
        experts_kernel,
        grid=(steps,),
        in_specs=[whole(xa), whole(xb), whole(wa), whole(wb)] + [into, into, back] * 2,
        out_specs=[pl.BlockSpec((rows, width), lambda i: (0, 0))] * 2,
        out_shape=[jax.ShapeDtypeStruct((rows, width), jnp.bfloat16)] * 2,
        scratch_shapes=[pltpu.VMEM((2 * rows, width), jnp.float32)],
        compiler_params=pltpu.CompilerParams(vmem_limit_bytes=32 << 20),
        cost_estimate=pl.CostEstimate(
            flops=24 * rows * width * units,
            bytes_accessed=12 * width * units + 16 * rows * width,
            transcendentals=4 * rows * units,
        ),
        name="experts",
    )(xa, xb, wa, wb, *weights)


def split_exact(value):
    parts = []
    for _ in range(3):
        part = lax.reduce_precision(value, 8, 7)
        parts.append(part.astype(jnp.bfloat16))
        value = value - part
    return jnp.concatenate(parts, axis=1)


def dense_on_device(
    query_plain,
    query_turn,
    latent,
    key_turn,
    latent_norm_scale,
    plain_key_matrix,
    value_matrix,
    residual,
    out_weight,
    ffn_gain,
    gate_weight,
    up_weight,
    down_weight,
    routes,
    route_weights,
):
    tok_dev = latent.shape[0]
    rows_dev = residual.shape[0]
    size = lax.axis_size("sp")
    count_experts = size * gate_weight.shape[0]
    me = lax.axis_index("sp")
    side = lax.axis_index("tp")
    core = me % 2
    chip = me // 2
    chips = size // 2
    heads_dev = query_plain.shape[1] // PLAIN_HEAD_WIDTH

    ids = jnp.arange(count_experts, dtype=jnp.int32)
    spread = jnp.sum(
        jnp.where(routes[:, :, None] == ids[None, None, :], route_weights[:, :, None], 0.0), axis=1
    )
    parts = split_exact(spread)
    spare = 128 - QK_ROPE
    parts = jnp.pad(parts, ((0, tok_dev - rows_dev), (0, spare - parts.shape[1])))
    packed = jnp.concatenate([latent, key_turn, parts], axis=1)

    one = zshift(packed, 1)
    three = zshift(packed, -1)
    two = zshift(one, 1)
    pieces = [packed, one, three, two]
    partners = [cswap(p) for p in pieces]
    slabs = [chip, (chip - 1) % chips, (chip + 1) % chips, (chip - 2) % chips]

    own_weights = (gate_weight[0], up_weight[0], down_weight[0])
    weights = own_weights + tuple(cswap(w) for w in own_weights)

    table = turn_table(jnp.arange(size * tok_dev, dtype=jnp.int32))
    own_table = lax.dynamic_slice_in_dim(table, me * tok_dev, tok_dev, 0)
    own_cos = jnp.tile(own_table[:, :QK_ROPE], (1, heads_dev))
    own_sin = jnp.tile(own_table[:, QK_ROPE:], (1, heads_dev))
    swapped = jnp.dot(
        query_turn, swap_matrix(query_turn.shape[1]), preferred_element_type=jnp.float32
    )
    query_rot = (query_turn.astype(jnp.float32) * own_cos + swapped * own_sin).astype(jnp.bfloat16)

    perm = swap_matrix(QK_ROPE)
    gain = latent_norm_scale[None, :]
    state = (jnp.zeros((8, 128), jnp.float32), jnp.zeros((8, 128), jnp.float32))
    for index in range(4):
        at = jnp.stack(
            [slabs[index] * 2 + core, slabs[index] * 2 + 1 - core, side]
        ).astype(jnp.int32)
        state = attend(
            index == 0,
            index == 3,
            at,
            query_plain,
            query_rot,
            pieces[index],
            partners[index],
            table,
            gain,
            plain_key_matrix,
            value_matrix,
            perm,
            *state,
        )
    mine, other = state
    arrived = xswap(other)
    hidden, normed = make_hidden(at, mine, arrived, out_weight, residual, ffn_gain[None, :])

    own_parts = jnp.concatenate(
        [p[:rows_dev, tok_dev * 0 + latent.shape[1] + QK_ROPE :] for p in pieces], axis=0
    )
    both = jnp.stack([own_parts, xswap(own_parts)])
    wide = both.astype(jnp.float32)
    full = sum(
        wide[:, :, i * count_experts : (i + 1) * count_experts] for i in range(3)
    )
    pick = jnp.stack([ids == me, ids == (me ^ 1)], axis=1).astype(jnp.float32)
    scales = jnp.sum(full[:, :, :, None] * pick[None, None], axis=2)
    scales = scales.reshape(2, 4, rows_dev, 2)

    d_one = zshift(normed, 1)
    d_three = zshift(normed, -1)
    d_two = zshift(d_one, 1)
    results = []
    for index, rows in enumerate((normed, d_one, d_three, d_two)):
        results.append(
            experts(rows, xswap(rows), scales[0, index], scales[1, index], weights)
        )

    def joined(pair):
        keep, send = pair
        return keep.astype(jnp.float32) + xswap(send).astype(jnp.float32)

    back_two = zshift(joined(results[3]).astype(jnp.bfloat16), -1)
    back_one = zshift(
        (joined(results[1]) + back_two.astype(jnp.float32)).astype(jnp.bfloat16), -1
    )
    back_three = zshift(joined(results[2]).astype(jnp.bfloat16), 1)
    return (
        hidden.astype(jnp.float32)
        + joined(results[0])
        + back_one.astype(jnp.float32)
        + back_three.astype(jnp.float32)
    ).astype(jnp.bfloat16)


def solution(mesh):
    sizes = dict(mesh.shape)
    small = sizes["sp"] == 8 and sizes["tp"] == 2
    on_device = dense_on_device if small else routed_on_device
    placed = (
        P(("grp", "sp"), "tp"),
        P(("grp", "sp"), "tp"),
        P(("grp", "sp"), None),
        P(("grp", "sp"), None),
        P(),
        P(None, "tp"),
        P(None, "tp"),
        P(("grp", "sp", "tp"), None),
        P(),
        P(),
        P("sp", None, "tp"),
        P("sp", None, "tp"),
        P("sp", "tp", None),
        P(("grp", "sp", "tp"), None),
        P(("grp", "sp", "tp"), None),
    )
    return jax.shard_map(
        on_device,
        mesh=mesh,
        in_specs=placed,
        out_specs=P(("grp", "sp", "tp"), None),
        check_vma=False,
    )
```
